32 devices in a mesh: grp: 2 (over y), kv: 4 (over z), tp: 4 (over x, core).
Axes of the slice: x: 2, y: 2, z: 4, core: 2. Of those that a mesh axis runs over, the one named last changes fastest.
Arguments:
- tokens: bfloat16 [32, 4096], P('grp', 'kv'), parts along dimension 0, may hold values from -16 to 16
- positions: int32 [32], P(('grp', 'kv')), parts along dimension 0, may hold values from 512 to 8191
- state: float32 [32, 16, 128, 128], P(('grp', 'kv'), 'tp'), parts along dimension 0, may hold values from -3 to 3
- norm_gain: float32 [4096], P('kv'), may hold values from 0.1 to 1.9
- w_query: bfloat16 [4096, 2048], P('kv', 'tp'), may hold values from -0.09375 to 0.09375
- w_key: bfloat16 [4096, 2048], P('kv', 'tp'), may hold values from -0.09375 to 0.09375
- w_value: bfloat16 [4096, 2048], P('kv', 'tp'), may hold values from -0.09375 to 0.09375
- w_gate: bfloat16 [4096, 2048], P('kv', 'tp'), may hold values from -0.09375 to 0.09375
- w_out: bfloat16 [2048, 4096], P('tp', 'kv'), may hold values from -0.125 to 0.125
- mlp_gain: float32 [4096], P('kv'), may hold values from 0.1 to 1.9
- w_up: bfloat16 [4096, 16384], P('kv', 'tp'), may hold values from -0.09375 to 0.09375
- w_down: bfloat16 [16384, 4096], P('tp', 'kv'), may hold values from -0.046875 to 0.046875
Outputs:
- layer_out: bfloat16 [32, 4096], P('grp', 'kv'), parts along dimension 0
- new_state: float32 [32, 16, 128, 128], P(('grp', 'kv'), 'tp'), parts along dimension 0
The draws below stay inside these ranges and needn't reach their ends.
There are 2 independent parts, one for each index of `grp`. The reference program is written for one: setup_inputs(seed, part) draws one part's arguments, and reference() takes and returns one part's arrays. A program takes and returns all parts, laid end to end along the dimension named above; an argument that names none is the same for every part. Nothing has to cross between parts.
All inputs are finite; a program needn't handle non-finite values.
Results may differ from the reference program's by a relative error of at most 0.007.
Values may be sent and summed in bfloat16 or wider, within the bound.
A program may use at most 64 MiB of HBM per device.

```python
import jax
import jax.numpy as jnp
from jax import lax

D = 4096
HEADS = 16
HEAD_DIM = 128
FF = 16384
BATCH = 16
RET = 2048


def draw_tokens(key, part):
    first = jax.random.fold_in(jax.random.fold_in(key, 11), 0)
    columns = jnp.exp(jnp.log(4.0) * jnp.arange(D, dtype=jnp.float32) / D) * 0.5
    base = jnp.clip(jax.random.normal(first, (BATCH, D), jnp.float32), -4.0, 4.0)
    values = base * columns[None, :]
    return values.astype(jnp.bfloat16)


def with_ends(values, own_key, low, top_value):
    longest = values.shape.index(max(values.shape))
    spots = []
    for shift in (0, 1):
        where = [jax.random.randint(jax.random.fold_in(own_key, axis), (), 0, length) for axis, length in enumerate(values.shape)]
        where[longest] = (where[longest] + shift) % values.shape[longest]
        spots.append(tuple(where))
    return values.at[spots[0]].set(low).at[spots[1]].set(top_value)


def block_scale(rng, shape, pieces, least, largest):
    def one(axis_at, blocks):
        steps = jax.random.uniform(jax.random.fold_in(jax.random.fold_in(rng, 6), axis_at), (blocks,), jnp.float32, least / len(pieces), largest / len(pieces))
        return jnp.repeat(jnp.exp(steps), shape[axis_at] // blocks).reshape((-1,) + (1,) * (len(shape) - axis_at - 1))

    level = one(*pieces[0])
    for cut in pieces[1:]:
        level = level * one(*cut)
    return level


def centred(key, dims, deviation, most, pieces=(), kind=jnp.bfloat16):
    values = deviation * jax.random.normal(key, dims, jnp.float32)
    if pieces:
        values = values * block_scale(key, dims, pieces, -0.22, 0.18)
    return jnp.clip(values, -most, most).astype(kind)


def setup_inputs(seed: int = 0, part: int = 0) -> dict:
    splits = jax.random.split(jax.random.key(seed), 13)
    part_keys = jax.random.split(jax.random.fold_in(splits[12], part), 13)
    tokens = draw_tokens(jax.random.fold_in(jax.random.fold_in(splits[12], part), 71), part)
    positions = with_ends(jax.random.randint(part_keys[1], (BATCH,), 512, 8192), jax.random.fold_in(part_keys[1], 1), 512, 8191).astype(jnp.int32)
    state = centred(part_keys[2], (BATCH, HEADS, HEAD_DIM, HEAD_DIM), 0.5, 3.0, ((0, 4), (1, 4)), jnp.float32)
    norm_gain = jnp.clip(1.0 + 0.18 * jax.random.normal(splits[3], (D,), jnp.float32), 0.1, 1.9)
    w_query = centred(splits[4], (D, RET), D ** -0.5, 0.09375, ((0, 4), (1, 4)))
    w_key = centred(splits[5], (D, RET), D ** -0.5, 0.09375, ((0, 4), (1, 4)))
    w_value = centred(splits[6], (D, RET), D ** -0.5, 0.09375, ((0, 4), (1, 4)))
    w_gate = centred(splits[7], (D, RET), D ** -0.5, 0.09375, ((0, 4), (1, 4)))
    w_out = centred(splits[8], (RET, D), RET ** -0.5, 0.125, ((0, 4), (1, 4)))
    mlp_gain = jnp.clip(1.0 + 0.18 * jax.random.normal(splits[9], (D,), jnp.float32), 0.1, 1.9)
    w_up = centred(splits[10], (D, FF), D ** -0.5, 0.09375, ((0, 4), (1, 4)))
    w_down = centred(splits[11], (FF, D), FF ** -0.5, 0.046875, ((0, 4), (1, 4)))
    return dict(tokens=tokens, positions=positions, state=state, norm_gain=norm_gain, w_query=w_query, w_key=w_key, w_value=w_value, w_gate=w_gate, w_out=w_out, mlp_gain=mlp_gain, w_up=w_up, w_down=w_down)


def turn(values, positions):
    half = values.shape[-1] // 2
    freq = 10000.0 ** (-(jnp.arange(half, dtype=jnp.float32) * 2.0) / values.shape[-1])
    angle = positions.astype(jnp.float32)[:, None, None] * freq[None, None, :]
    cosine = jnp.cos(angle)
    sine = jnp.sin(angle)
    first = values[..., :half]
    second = values[..., half:]
    return jnp.concatenate([first * cosine - second * sine, first * sine + second * cosine], axis=-1)

def reference(tokens, positions, state, norm_gain, w_query, w_key, w_value, w_gate, w_out, mlp_gain, w_up, w_down):
    rows = tokens.shape[0]
    inputs = tokens.astype(jnp.float32)
    scale1 = lax.rsqrt(lax.optimization_barrier(jnp.mean(inputs * inputs, axis=1)) + 1e-06)
    normed = (inputs * norm_gain).astype(jnp.bfloat16)

    def project(weight):
        raw = jnp.dot(normed, weight, preferred_element_type=jnp.float32) * scale1[:, None]
        return raw.reshape(rows, HEADS, HEAD_DIM)
    query = turn(project(w_query), positions)
    key = turn(project(w_key), positions) * HEAD_DIM ** (-0.5)
    value = project(w_value)
    gate = project(w_gate)
    heads = jnp.arange(HEADS, dtype=jnp.float32)
    gamma = 1.0 - 2.0 ** (-5.0 - 5.0 * heads / (HEADS - 1))
    new_state = gamma[None, :, None, None] * state + key[:, :, :, None] * value[:, :, None, :]
    read = jnp.einsum('bhd,bhde->bhe', query, new_state, precision=lax.Precision.HIGHEST)
    read = read * lax.rsqrt(lax.optimization_barrier(jnp.mean(read * read, axis=-1, keepdims=True)) + 1e-06)
    retained = (read * jax.nn.silu(gate)).reshape(rows, HEADS * HEAD_DIM).astype(jnp.bfloat16)
    mixed = (inputs + jnp.dot(retained, w_out, preferred_element_type=jnp.float32)).astype(jnp.bfloat16)
    middle = mixed.astype(jnp.float32)
    scale2 = lax.rsqrt(lax.optimization_barrier(jnp.mean(middle * middle, axis=1)) + 1e-06)
    normed2 = (middle * mlp_gain).astype(jnp.bfloat16)
    upward = jnp.dot(normed2, w_up, preferred_element_type=jnp.float32) * scale2[:, None]
    hidden = jnp.square(jax.nn.relu(upward)).astype(jnp.bfloat16)
    layer_out = (middle + jnp.dot(hidden, w_down, preferred_element_type=jnp.float32)).astype(jnp.bfloat16)
    return (layer_out, new_state)
```

```python
import functools

import jax
import jax.numpy as jnp
import numpy as np
from jax import lax
from jax.experimental import pallas as pl
from jax.experimental.pallas import tpu as pltpu
from jax.sharding import PartitionSpec as P

D = 4096
HEADS = 16
MESH = pl.DeviceIdType.MESH
F32 = jnp.float32
BF16 = jnp.bfloat16


def tile_of(width):
    return 512 if width % 512 == 0 else (256 if width % 256 == 0 else 128)


def lane_fill(column):
    return jnp.broadcast_to(column, (column.shape[0], 128))


def split_high_low(column):
    high = column.astype(BF16)
    low = (column - high.astype(F32)).astype(BF16)
    return jnp.concatenate([lane_fill(high.astype(F32)), lane_fill(low.astype(F32))], axis=1)


def kernel(
    kv, tp, chunks,
    positions, tokens, state, norm_gain, freq, w_query, w_key, w_value, w_gate, w_out, mlp_gain, w_up, w_down,
    out_ref, new_state,
    tok_v, gain1_v, gain2_v, freq_v, wq_v, wk_v, wv_v, wg_v, wo_v, wu_v, wd_v, st_v,
    send1, recv1, ret, mix, send2, recv2, sums2, rsums2, hid, down, out_v,
    load_sem, s1_sem, r1_sem, sr_sem, rr_sem, sm_sem, rm_sem, s2_sem, r2_sem, ss_sem, rs_sem, sh_sem, rh_sem,
    sd_sem, rd_sem, store_sem,
):
    me_kv = lax.axis_index("kv")
    me_tp = lax.axis_index("tp")
    rows, width = tok_v.shape
    seqs = rows // kv
    ret_width = wq_v.shape[1]
    head_size = st_v.shape[-1]
    heads = st_v.shape[1]
    ff = wu_v.shape[1]
    cw = ff // chunks

    loads = []

    def load(src, dst):
        copy = pltpu.make_async_copy(src, dst, load_sem.at[len(loads)])
        loads.append(copy)
        copy.start()
        return copy

    l_tok = load(tokens, tok_v)
    l_g1 = load(norm_gain, gain1_v)
    l_w = [load(a, b) for a, b in ((w_query, wq_v), (w_key, wk_v), (w_value, wv_v), (w_gate, wg_v))]
    l_freq = load(freq, freq_v)
    l_state = load(state, st_v)
    l_wo = load(w_out, wo_v)
    l_g2 = load(mlp_gain, gain2_v)
    l_up = [load(w_up.at[:, pl.ds(c * cw, cw)], wu_v.at[:, pl.ds(c * cw, cw)]) for c in range(chunks)]
    l_down = [load(w_down.at[pl.ds(c * cw, cw), :], wd_v.at[pl.ds(c * cw, cw), :]) for c in range(chunks)]

    barrier = pltpu.get_barrier_semaphore()
    for s in range(1, kv):
        pl.semaphore_signal(barrier, inc=1, device_id={"kv": lax.rem(me_kv + s, kv)}, device_id_type=MESH)
    for s in range(1, tp):
        pl.semaphore_signal(barrier, inc=1, device_id={"tp": lax.rem(me_tp + s, tp)}, device_id_type=MESH)

    def remote(src, dst, send_sem, recv_sem, axis, target):
        copy = pltpu.make_async_remote_copy(
            src_ref=src, dst_ref=dst, send_sem=send_sem, recv_sem=recv_sem,
            device_id={axis: target}, device_id_type=MESH,
        )
        copy.start()
        return copy

    l_tok.wait()
    l_g1.wait()
    inputs = tok_v[...].astype(F32)
    normed = (inputs * gain1_v[...]).astype(BF16)
    extra = split_high_low(jnp.sum(inputs * inputs, axis=1, keepdims=True))
    for j in range(kv):
        send1[j, :, 4 * ret_width:] = extra[j * seqs:(j + 1) * seqs].astype(BF16)

    l_freq.wait()
    row = lax.broadcasted_iota(jnp.int32, (seqs, head_size), 0)
    lane = lax.broadcasted_iota(jnp.int32, (seqs, head_size), 1)
    pos = jnp.zeros((seqs, head_size), F32)
    for b in range(seqs):
        pos = jnp.where(row == b, positions[b].astype(F32), pos)
    angle = pos * freq_v[...]
    cosine = jnp.cos(angle)
    sine = jnp.where(lane < head_size // 2, -1.0, 1.0) * jnp.sin(angle)

    t1 = tile_of(ret_width)
    for i, weight in enumerate((wq_v, wk_v, wv_v, wg_v)):
        l_w[i].wait()
        for n in range(ret_width // t1):
            term = jnp.dot(normed, weight[:, n * t1:(n + 1) * t1], preferred_element_type=F32)
            at = i * ret_width + n * t1
            for j in range(kv):
                send1[j, :, at:at + t1] = term[j * seqs:(j + 1) * seqs].astype(BF16)

    pl.semaphore_wait(barrier, kv + tp - 2)
    pending = []
    copies = []
    for s in range(1, kv):
        to = lax.rem(me_kv + s, kv)
        copies.append(remote(send1.at[to], recv1.at[s - 1], s1_sem.at[s - 1], r1_sem.at[s - 1], "kv", to))
    pending += copies
    summed = send1[me_kv].astype(F32)
    for s in range(1, kv):
        copies[s - 1].wait_recv()
        summed = summed + recv1[s - 1].astype(F32)
    total = summed[:, 4 * ret_width:4 * ret_width + 1] + summed[:, 4 * ret_width + 128:4 * ret_width + 129]
    scale1 = lax.rsqrt(total / D + 1e-06)

    def stack(i):
        base = i * ret_width
        return jnp.concatenate(
            [summed[:, base + h * head_size:base + (h + 1) * head_size] * scale1 for h in range(heads)], axis=0
        )

    cos_all = jnp.concatenate([cosine] * heads, axis=0)
    sin_all = jnp.concatenate([sine] * heads, axis=0)

    def turn(x):
        return x * cos_all + pltpu.roll(x, head_size // 2, 1) * sin_all

    count = seqs * heads
    query = turn(stack(0))
    key = turn(stack(1)) * head_size ** (-0.5)
    value = stack(2)
    gate = stack(3)
    columns = jnp.transpose(
        jnp.concatenate([query, key, jnp.zeros((128 - 2 * count, head_size), F32)], axis=0)
    )
    l_state.wait()
    reads = []
    for h in range(heads):
        index = (me_tp * heads + h).astype(F32)
        gamma = 1.0 - jnp.exp2(jnp.full((1, head_size), -5.0, F32) - 5.0 * index / (HEADS - 1))
        for b in range(seqs):
            at = h * seqs + b
            fresh = gamma * st_v[b, h] + columns[:, count + at:count + at + 1] * value[at:at + 1, :]
            st_v[b, h] = fresh
            reads.append(jnp.sum(columns[:, at:at + 1] * fresh, axis=0, keepdims=True))
    read = jnp.concatenate(reads, axis=0)
    read = read * lax.rsqrt(jnp.mean(read * read, axis=-1, keepdims=True) + 1e-06)
    kept = read * (gate / (1.0 + jnp.exp(-gate)))
    for h in range(heads):
        ret[me_kv, :, h * head_size:(h + 1) * head_size] = kept[h * seqs:(h + 1) * seqs].astype(BF16)
    copies = []
    for s in range(1, kv):
        to = lax.rem(me_kv + s, kv)
        copies.append(remote(ret.at[me_kv], ret.at[me_kv], sr_sem.at[s - 1], rr_sem.at[s - 1], "kv", to))
    pending += copies
    store_state = pltpu.make_async_copy(st_v, new_state, store_sem.at[0])
    store_state.start()
    l_wo.wait()
    for s in range(1, kv):
        copies[s - 1].wait_recv()
    retained = jnp.concatenate([ret[j].astype(F32) for j in range(kv)], axis=0).astype(BF16)

    def reduce_tp(terms_into, buffer, send_sem, recv_sem):
        terms_into()
        sent = []
        for s in range(1, tp):
            to = lax.rem(me_tp + s, tp)
            sent.append(remote(buffer.at[me_tp], buffer.at[me_tp], send_sem.at[s - 1], recv_sem.at[s - 1], "tp", to))
        for s in range(1, tp):
            sent[s - 1].wait_recv()
        result = buffer[0].astype(F32)
        for j in range(1, tp):
            result = result + buffer[j].astype(F32)
        return result, sent

    t2 = tile_of(width)

    def out_terms():
        for n in range(width // t2):
            cols = slice(n * t2, (n + 1) * t2)
            mix[me_tp, :, cols] = jnp.dot(retained, wo_v[:, cols], preferred_element_type=F32).astype(BF16)

    head_sum, sent = reduce_tp(out_terms, mix, sm_sem, rm_sem)
    pending += sent
    mixed = (inputs + head_sum).astype(BF16)
    middle = mixed.astype(F32)
    l_g2.wait()
    normed2 = (middle * gain2_v[...]).astype(BF16)
    extra = split_high_low(jnp.sum(middle * middle, axis=1, keepdims=True))
    for j in range(kv):
        sums2[j] = extra[j * seqs:(j + 1) * seqs].astype(BF16)
    sum_copies = []
    for s in range(1, kv):
        to = lax.rem(me_kv + s, kv)
        sum_copies.append(remote(sums2.at[to], rsums2.at[s - 1], ss_sem.at[s - 1], rs_sem.at[s - 1], "kv", to))
    pending += sum_copies

    t3 = tile_of(cw)
    up_copies = []
    for c in range(chunks):
        l_up[c].wait()

        @pl.loop(0, cw // t3)
        def _(n, c=c):
            start = pl.multiple_of(n * t3, t3)
            term = jnp.dot(normed2, wu_v[:, pl.ds(c * cw + start, t3)], preferred_element_type=F32)
            for j in range(kv):
                send2[c, j, :, pl.ds(start, t3)] = term[j * seqs:(j + 1) * seqs].astype(BF16)

        row_copies = []
        for s in range(1, kv):
            to = lax.rem(me_kv + s, kv)
            row_copies.append(
                remote(send2.at[c, to], recv2.at[c, s - 1], s2_sem.at[c, s - 1], r2_sem.at[c, s - 1], "kv", to)
            )
        up_copies.append(row_copies)
        pending += row_copies

    sums = sums2[me_kv].astype(F32)
    for s in range(1, kv):
        sum_copies[s - 1].wait_recv()
        sums = sums + rsums2[s - 1].astype(F32)
    scale2 = lax.rsqrt((sums[:, :1] + sums[:, 128:129]) / D + 1e-06)

    hid_copies = []
    for c in range(chunks):
        up_sum = send2[c, me_kv].astype(F32)
        for s in range(1, kv):
            up_copies[c][s - 1].wait_recv()
            up_sum = up_sum + recv2[c, s - 1].astype(F32)
        positive = jnp.maximum(up_sum * scale2, 0.0)
        hid[c, me_kv] = (positive * positive).astype(BF16)
        row_copies = []
        for s in range(1, kv):
            to = lax.rem(me_kv + s, kv)
            row_copies.append(
                remote(hid.at[c, me_kv], hid.at[c, me_kv], sh_sem.at[c, s - 1], rh_sem.at[c, s - 1], "kv", to)
            )
        hid_copies.append(row_copies)
        pending += row_copies

    for c in range(chunks):
        l_down[c].wait()
        for s in range(1, kv):
            hid_copies[c][s - 1].wait_recv()
        hidden = jnp.concatenate([hid[c, j].astype(F32) for j in range(kv)], axis=0).astype(BF16)

        @pl.loop(0, width // t2)
        def _(n, c=c, hidden=hidden):
            cols = pl.ds(pl.multiple_of(n * t2, t2), t2)
            term = jnp.dot(hidden, wd_v[pl.ds(c * cw, cw), cols], preferred_element_type=F32)
            if c == 0:
                out_v[:, cols] = term
            else:
                out_v[:, cols] += term

    def down_terms():
        down[me_tp] = out_v[...].astype(BF16)

    down_sum, sent = reduce_tp(down_terms, down, sd_sem, rd_sem)
    pending += sent
    out_ref[...] = (middle + down_sum).astype(BF16)
    for copy in pending:
        copy.wait_send()
    store_state.wait()


def solution(mesh):
    kv, tp = mesh.shape["kv"], mesh.shape["tp"]

    def shards(
        tokens, positions, state, norm_gain, w_query, w_key, w_value, w_gate, w_out, mlp_gain, w_up, w_down
    ):
        rows, width = tokens.shape
        seqs, heads, head_size, _ = state.shape
        ret_width = w_query.shape[1]
        ff = w_up.shape[1]
        chunks = 4
        cw = ff // chunks
        half = head_size // 2
        table = 10000.0 ** (-(np.arange(half) * 2.0) / head_size)
        freq = jnp.asarray(np.concatenate([table, table])[None, :], F32)
        any_spec = pl.BlockSpec(memory_space=pl.ANY)
        vmem = pltpu.VMEM
        dma = pltpu.SemaphoreType.DMA
        block1 = 4 * ret_width + 256
        return pl.pallas_call(
            functools.partial(kernel, kv, tp, chunks),
            name="layer",
            out_shape=(
                jax.ShapeDtypeStruct((rows, width), BF16),
                jax.ShapeDtypeStruct(state.shape, F32),
            ),
            in_specs=[pl.BlockSpec(memory_space=pltpu.SMEM)] + [any_spec] * 12,
            out_specs=(pl.BlockSpec(memory_space=pltpu.VMEM), any_spec),
            scratch_shapes=[
                vmem((rows, width), BF16),
                vmem((1, width), F32),
                vmem((1, width), F32),
                vmem((1, head_size), F32),
                vmem(w_query.shape, BF16),
                vmem(w_key.shape, BF16),
                vmem(w_value.shape, BF16),
                vmem(w_gate.shape, BF16),
                vmem(w_out.shape, BF16),
                vmem(w_up.shape, BF16),
                vmem(w_down.shape, BF16),
                vmem(state.shape, F32),
                vmem((kv, seqs, block1), BF16),
                vmem((kv - 1, seqs, block1), BF16),
                vmem((kv, seqs, ret_width), BF16),
                vmem((tp, rows, width), BF16),
                vmem((chunks, kv, seqs, cw), BF16),
                vmem((chunks, kv - 1, seqs, cw), BF16),
                vmem((kv, seqs, 256), BF16),
                vmem((kv - 1, seqs, 256), BF16),
                vmem((chunks, kv, seqs, cw), BF16),
                vmem((tp, rows, width), BF16),
                vmem((rows, width), F32),
                dma((10 + 2 * chunks,)),
                dma((kv - 1,)), dma((kv - 1,)),
                dma((kv - 1,)), dma((kv - 1,)),
                dma((tp - 1,)), dma((tp - 1,)),
                dma((chunks, kv - 1)), dma((chunks, kv - 1)),
                dma((kv - 1,)), dma((kv - 1,)),
                dma((chunks, kv - 1)), dma((chunks, kv - 1)),
                dma((tp - 1,)), dma((tp - 1,)),
                dma((1,)),
            ],
            compiler_params=pltpu.CompilerParams(
                collective_id=0, has_side_effects=True, vmem_limit_bytes=60 * 1024 * 1024
            ),
        )(
            positions, tokens, state, norm_gain[None, :], freq, w_query, w_key, w_value, w_gate, w_out,
            mlp_gain[None, :], w_up, w_down,
        )

    return jax.shard_map(
        shards,
        mesh=mesh,
        in_specs=(
            P("grp", "kv"),
            P(("grp", "kv")),
            P(("grp", "kv"), "tp", None, None),
            P("kv"),
            P("kv", "tp"),
            P("kv", "tp"),
            P("kv", "tp"),
            P("kv", "tp"),
            P("tp", "kv"),
            P("kv"),
            P("kv", "tp"),
            P("tp", "kv"),
        ),
        out_specs=(P("grp", "kv"), P(("grp", "kv"), "tp", None, None)),
        check_vma=False,
    )
```

```python
import functools

import jax
import jax.numpy as jnp
import numpy as np
from jax import lax
from jax.experimental import pallas as pl
from jax.experimental.pallas import tpu as pltpu
from jax.sharding import PartitionSpec as P

D = 4096
HEADS = 16
MESH = pl.DeviceIdType.MESH
F32 = jnp.float32
BF16 = jnp.bfloat16


def tile_of(width):
    return 512 if width % 512 == 0 else (256 if width % 256 == 0 else 128)


def lane_fill(column):
    return jnp.broadcast_to(column, (column.shape[0], 128))


def split_high_low(column):
    high = column.astype(BF16)
    low = (column - high.astype(F32)).astype(BF16)
    return jnp.concatenate([lane_fill(high.astype(F32)), lane_fill(low.astype(F32))], axis=1)


def kernel(
    kv, tp, chunks,
    positions, tokens, state, norm_gain, freq, w_query, w_key, w_value, w_gate, w_out, mlp_gain, w_up, w_down,
    out_ref, st_v,
    pos_s, tok_v, gain1_v, gain2_v, freq_v, wq_v, wk_v, wv_v, wg_v, wo_v, wu_v, wd_v,
    send1, recv1, ret, mix, send2, recv2, sums2, rsums2, hid, down, out_v,
    load_sem, s1_sem, r1_sem, sr_sem, rr_sem, sm_sem, rm_sem, s2_sem, r2_sem, ss_sem, rs_sem, sh_sem, rh_sem,
    sd_sem, rd_sem,
):
    me_kv = lax.axis_index("kv")
    me_tp = lax.axis_index("tp")
    rows, width = tok_v.shape
    seqs = rows // kv
    ret_width = wq_v.shape[1]
    head_size = st_v.shape[-1]
    heads = st_v.shape[1]
    ff = wu_v.shape[1]
    cw = ff // chunks

    loads = []

    def load(src, dst):
        copy = pltpu.make_async_copy(src, dst, load_sem.at[len(loads)])
        loads.append(copy)
        copy.start()
        return copy

    l_tok = load(tokens, tok_v)
    l_g1 = load(norm_gain, gain1_v)
    l_w = [load(a, b) for a, b in ((w_query, wq_v), (w_key, wk_v), (w_value, wv_v), (w_gate, wg_v))]
    l_freq = load(freq, freq_v)
    l_pos = load(positions, pos_s)
    l_state = load(state, st_v)
    l_wo = load(w_out, wo_v)
    l_g2 = load(mlp_gain, gain2_v)
    l_up = [load(w_up.at[:, pl.ds(c * cw, cw)], wu_v.at[:, pl.ds(c * cw, cw)]) for c in range(chunks)]
    l_down = [load(w_down.at[pl.ds(c * cw, cw), :], wd_v.at[pl.ds(c * cw, cw), :]) for c in range(chunks)]

    barrier = pltpu.get_barrier_semaphore()
    for s in range(1, kv):
        pl.semaphore_signal(barrier, inc=1, device_id={"kv": lax.rem(me_kv + s, kv)}, device_id_type=MESH)
    for s in range(1, tp):
        pl.semaphore_signal(barrier, inc=1, device_id={"tp": lax.rem(me_tp + s, tp)}, device_id_type=MESH)

    def remote(src, dst, send_sem, recv_sem, axis, target):
        copy = pltpu.make_async_remote_copy(
            src_ref=src, dst_ref=dst, send_sem=send_sem, recv_sem=recv_sem,
            device_id={axis: target}, device_id_type=MESH,
        )
        copy.start()
        return copy

    l_tok.wait()
    l_g1.wait()
    inputs = tok_v[...].astype(F32)
    normed = (inputs * gain1_v[...]).astype(BF16)
    extra = split_high_low(jnp.sum(inputs * inputs, axis=1, keepdims=True))
    for j in range(kv):
        send1[0, j, :, 2 * ret_width:] = extra[j * seqs:(j + 1) * seqs].astype(BF16)

    l_freq.wait()
    l_pos.wait()
    row = lax.broadcasted_iota(jnp.int32, (seqs, head_size), 0)
    lane = lax.broadcasted_iota(jnp.int32, (seqs, head_size), 1)
    pos = jnp.zeros((seqs, head_size), F32)
    for b in range(seqs):
        pos = jnp.where(row == b, pos_s[b].astype(F32), pos)
    angle = pos * freq_v[...]
    cosine = jnp.cos(angle)
    sine = jnp.where(lane < head_size // 2, -1.0, 1.0) * jnp.sin(angle)

    t1 = tile_of(ret_width)
    copies = ([], [])
    for i, weight in enumerate((wq_v, wk_v, wv_v, wg_v)):
        l_w[i].wait()
        for n in range(ret_width // t1):
            term = jnp.dot(normed, weight[:, n * t1:(n + 1) * t1], preferred_element_type=F32)
            at = (i % 2) * ret_width + n * t1
            for j in range(kv):
                send1[i // 2, j, :, at:at + t1] = term[j * seqs:(j + 1) * seqs].astype(BF16)
        if i % 2 == 1:
            if i == 1:
                pl.semaphore_wait(barrier, kv + tp - 2)
            p = i // 2
            piece = pl.ds(0, 2 * ret_width + (256 if p == 0 else 0))
            for s in range(1, kv):
                to = lax.rem(me_kv + s, kv)
                copies[p].append(
                    remote(
                        send1.at[p, to, :, piece], recv1.at[p, s - 1, :, piece],
                        s1_sem.at[p, s - 1], r1_sem.at[p, s - 1], "kv", to,
                    )
                )
    pending = copies[0] + copies[1]

    def gathered(p, size):
        result = send1[p, me_kv, :, :size].astype(F32)
        for s in range(1, kv):
            copies[p][s - 1].wait_recv()
            result = result + recv1[p, s - 1, :, :size].astype(F32)
        return result

    summed = gathered(0, 2 * ret_width + 256)
    total = summed[:, 2 * ret_width:2 * ret_width + 1] + summed[:, 2 * ret_width + 128:2 * ret_width + 129]
    scale1 = lax.rsqrt(total / D + 1e-06)

    def stack(values, i):
        base = i * ret_width
        return jnp.concatenate(
            [values[:, base + h * head_size:base + (h + 1) * head_size] * scale1 for h in range(heads)], axis=0
        )

    cos_all = jnp.concatenate([cosine] * heads, axis=0)
    sin_all = jnp.concatenate([sine] * heads, axis=0)

    def turn(x):
        return x * cos_all + pltpu.roll(x, head_size // 2, 1) * sin_all

    count = seqs * heads
    query = turn(stack(summed, 0))
    key = turn(stack(summed, 1)) * head_size ** (-0.5)
    columns = jnp.transpose(
        jnp.concatenate([query, key, jnp.zeros((128 - 2 * count, head_size), F32)], axis=0)
    )
    overlap = jnp.sum(query * key, axis=1, keepdims=True)
    gammas = [
        1.0 - jnp.exp2(jnp.full((1, head_size), -5.0, F32) - 5.0 * (me_tp * heads + h).astype(F32) / (HEADS - 1))
        for h in range(heads)
    ]
    l_state.wait()
    old_reads = []
    for h in range(heads):
        for b in range(seqs):
            at = h * seqs + b
            old_reads.append(gammas[h] * jnp.sum(columns[:, at:at + 1] * st_v[b, h], axis=0, keepdims=True))
    old_read = jnp.concatenate(old_reads, axis=0)
    summed = gathered(1, 2 * ret_width)
    value = stack(summed, 0)
    gate = stack(summed, 1)
    read = old_read + overlap * value
    read = read * lax.rsqrt(jnp.mean(read * read, axis=-1, keepdims=True) + 1e-06)
    kept = read * (gate / (1.0 + jnp.exp(-gate)))
    for h in range(heads):
        ret[me_kv, :, h * head_size:(h + 1) * head_size] = kept[h * seqs:(h + 1) * seqs].astype(BF16)
    copies = []
    for s in range(1, kv):
        to = lax.rem(me_kv + s, kv)
        copies.append(remote(ret.at[me_kv], ret.at[me_kv], sr_sem.at[s - 1], rr_sem.at[s - 1], "kv", to))
    pending += copies
    for h in range(heads):
        for b in range(seqs):
            at = h * seqs + b
            st_v[b, h] = gammas[h] * st_v[b, h] + columns[:, count + at:count + at + 1] * value[at:at + 1, :]

    t2 = tile_of(width)
    l_wo.wait()
    mix_copies = []
    for r in range(kv):
        owner = lax.rem(me_kv + kv - r, kv)
        if r > 0:
            copies[r - 1].wait_recv()
        block = ret[owner]
        for n in range(width // t2):
            cols = slice(n * t2, (n + 1) * t2)
            mix[me_tp, owner, :, cols] = jnp.dot(block, wo_v[:, cols], preferred_element_type=F32).astype(BF16)
        row_copies = []
        for s in range(1, tp):
            to = lax.rem(me_tp + s, tp)
            row_copies.append(
                remote(
                    mix.at[me_tp, owner], mix.at[me_tp, owner], sm_sem.at[r, s - 1], rm_sem.at[r, s - 1], "tp", to
                )
            )
        mix_copies.append(row_copies)
        pending += row_copies
    for row_copies in mix_copies:
        for copy in row_copies:
            copy.wait_recv()

    def added(j):
        return jnp.concatenate([mix[j, k].astype(F32) for k in range(kv)], axis=0)

    head_sum = added(0)
    for j in range(1, tp):
        head_sum = head_sum + added(j)
    mixed = (inputs + head_sum).astype(BF16)
    middle = mixed.astype(F32)
    l_g2.wait()
    normed2 = (middle * gain2_v[...]).astype(BF16)
    extra = split_high_low(jnp.sum(middle * middle, axis=1, keepdims=True))
    for j in range(kv):
        sums2[j] = extra[j * seqs:(j + 1) * seqs].astype(BF16)
    sum_copies = []
    for s in range(1, kv):
        to = lax.rem(me_kv + s, kv)
        sum_copies.append(remote(sums2.at[to], rsums2.at[s - 1], ss_sem.at[s - 1], rs_sem.at[s - 1], "kv", to))
    pending += sum_copies

    t3 = tile_of(cw)
    up_copies = []
    for c in range(chunks):
        l_up[c].wait()

        @pl.loop(0, cw // t3)
        def _(n, c=c):
            start = pl.multiple_of(n * t3, t3)
            term = jnp.dot(normed2, wu_v[:, pl.ds(c * cw + start, t3)], preferred_element_type=F32)
            for j in range(kv):
                send2[c, j, :, pl.ds(start, t3)] = term[j * seqs:(j + 1) * seqs].astype(BF16)

        row_copies = []
        for s in range(1, kv):
            to = lax.rem(me_kv + s, kv)
            row_copies.append(
                remote(send2.at[c, to], recv2.at[c, s - 1], s2_sem.at[c, s - 1], r2_sem.at[c, s - 1], "kv", to)
            )
        up_copies.append(row_copies)
        pending += row_copies

    sums = sums2[me_kv].astype(F32)
    for s in range(1, kv):
        sum_copies[s - 1].wait_recv()
        sums = sums + rsums2[s - 1].astype(F32)
    scale2 = lax.rsqrt((sums[:, :1] + sums[:, 128:129]) / D + 1e-06)

    hid_copies = []
    for c in range(chunks):
        up_sum = send2[c, me_kv].astype(F32)
        for s in range(1, kv):
            up_copies[c][s - 1].wait_recv()
            up_sum = up_sum + recv2[c, s - 1].astype(F32)
        positive = jnp.maximum(up_sum * scale2, 0.0)
        hid[c, me_kv] = (positive * positive).astype(BF16)
        row_copies = []
        for s in range(1, kv):
            to = lax.rem(me_kv + s, kv)
            row_copies.append(
                remote(hid.at[c, me_kv], hid.at[c, me_kv], sh_sem.at[c, s - 1], rh_sem.at[c, s - 1], "kv", to)
            )
        hid_copies.append(row_copies)
        pending += row_copies

    last = []
    for c in range(chunks):
        l_down[c].wait()
        for s in range(1, kv):
            hid_copies[c][s - 1].wait_recv()
        hidden = jnp.concatenate([hid[c, j].astype(F32) for j in range(kv)], axis=0).astype(BF16)
        for n in range(width // t2):
            cols = slice(n * t2, (n + 1) * t2)
            term = jnp.dot(hidden, wd_v[c * cw:(c + 1) * cw, cols], preferred_element_type=F32)
            if c > 0:
                term = term + out_v[:, cols]
            if c < chunks - 1:
                out_v[:, cols] = term
                continue
            down[me_tp, n] = term.astype(BF16)
            row_copies = []
            for s in range(1, tp):
                to = lax.rem(me_tp + s, tp)
                row_copies.append(
                    remote(
                        down.at[me_tp, n], down.at[me_tp, n], sd_sem.at[n, s - 1], rd_sem.at[n, s - 1], "tp", to
                    )
                )
            last.append(row_copies)
            pending += row_copies
    for n in range(width // t2):
        for copy in last[n]:
            copy.wait_recv()
        total = down[0, n].astype(F32)
        for j in range(1, tp):
            total = total + down[j, n].astype(F32)
        cols = slice(n * t2, (n + 1) * t2)
        out_ref[:, cols] = (middle[:, cols] + total).astype(BF16)
    for copy in pending:
        copy.wait_send()


def finish(made, fresh, out_ref, new_state, sem):
    first = pltpu.make_async_copy(fresh, new_state, sem.at[0])
    second = pltpu.make_async_copy(made, out_ref, sem.at[1])
    first.start()
    second.start()
    first.wait()
    second.wait()


def solution(mesh):
    kv, tp = mesh.shape["kv"], mesh.shape["tp"]

    def shards(
        tokens, positions, state, norm_gain, w_query, w_key, w_value, w_gate, w_out, mlp_gain, w_up, w_down
    ):
        rows, width = tokens.shape
        seqs, heads, head_size, _ = state.shape
        ret_width = w_query.shape[1]
        ff = w_up.shape[1]
        chunks = 4
        cw = ff // chunks
        half = head_size // 2
        table = 10000.0 ** (-(np.arange(half) * 2.0) / head_size)
        freq = jnp.asarray(np.concatenate([table, table])[None, :], F32)
        any_spec = pl.BlockSpec(memory_space=pltpu.HBM)
        vmem = pltpu.VMEM
        dma = pltpu.SemaphoreType.DMA
        block1 = 2 * ret_width + 256
        parts = width // tile_of(width)
        made, fresh = pl.pallas_call(
            functools.partial(kernel, kv, tp, chunks),
            name="layer",
            out_shape=(
                pltpu.VMEM((rows, width), BF16),
                pltpu.VMEM(state.shape, F32),
            ),
            in_specs=[any_spec] * 13,
            out_specs=(pl.BlockSpec(memory_space=pltpu.VMEM), pl.BlockSpec(memory_space=pltpu.VMEM)),
            scratch_shapes=[
                pltpu.SMEM(positions.shape, jnp.int32),
                vmem((rows, width), BF16),
                vmem((1, width), F32),
                vmem((1, width), F32),
                vmem((1, head_size), F32),
                vmem(w_query.shape, BF16),
                vmem(w_key.shape, BF16),
                vmem(w_value.shape, BF16),
                vmem(w_gate.shape, BF16),
                vmem(w_out.shape, BF16),
                vmem(w_up.shape, BF16),
                vmem(w_down.shape, BF16),
                vmem((2, kv, seqs, block1), BF16),
                vmem((2, kv - 1, seqs, block1), BF16),
                vmem((kv, seqs, ret_width), BF16),
                vmem((tp, kv, seqs, width), BF16),
                vmem((chunks, kv, seqs, cw), BF16),
                vmem((chunks, kv - 1, seqs, cw), BF16),
                vmem((kv, seqs, 256), BF16),
                vmem((kv - 1, seqs, 256), BF16),
                vmem((chunks, kv, seqs, cw), BF16),
                vmem((tp, parts, rows, width // parts), BF16),
                vmem((rows, width), F32),
                dma((11 + 2 * chunks,)),
                dma((2, kv - 1)), dma((2, kv - 1)),
                dma((kv - 1,)), dma((kv - 1,)),
                dma((kv, tp - 1)), dma((kv, tp - 1)),
                dma((chunks, kv - 1)), dma((chunks, kv - 1)),
                dma((kv - 1,)), dma((kv - 1,)),
                dma((chunks, kv - 1)), dma((chunks, kv - 1)),
                dma((parts, tp - 1)), dma((parts, tp - 1)),
            ],
            compiler_params=pltpu.CompilerParams(
                collective_id=0, has_side_effects=True, vmem_limit_bytes=48 * 1024 * 1024
            ),
        )(
            *[
                pltpu.with_memory_space_constraint(x, pltpu.HBM)
                for x in (
                    positions, tokens, state, norm_gain[None, :], freq, w_query, w_key, w_value, w_gate, w_out,
                    mlp_gain[None, :], w_up, w_down,
                )
            ],
        )
        return pl.pallas_call(
            finish,
            name="finish",
            out_shape=(
                jax.ShapeDtypeStruct((rows, width), BF16),
                jax.ShapeDtypeStruct(state.shape, F32),
            ),
            in_specs=[pl.BlockSpec(memory_space=pltpu.VMEM)] * 2,
            out_specs=(any_spec, any_spec),
            scratch_shapes=[pltpu.SemaphoreType.DMA((2,))],
            compiler_params=pltpu.CompilerParams(vmem_limit_bytes=4 * 1024 * 1024),
        )(made, fresh)

    return jax.shard_map(
        shards,
        mesh=mesh,
        in_specs=(
            P("grp", "kv"),
            P(("grp", "kv")),
            P(("grp", "kv"), "tp", None, None),
            P("kv"),
            P("kv", "tp"),
            P("kv", "tp"),
            P("kv", "tp"),
            P("kv", "tp"),
            P("tp", "kv"),
            P("kv"),
            P("kv", "tp"),
            P("tp", "kv"),
        ),
        out_specs=(P("grp", "kv"), P(("grp", "kv"), "tp", None, None)),
        check_vma=False,
    )
```

```python
import functools

import jax
import jax.numpy as jnp
import numpy as np
from jax import lax
from jax.experimental import pallas as pl
from jax.experimental.pallas import tpu as pltpu
from jax.sharding import PartitionSpec as P

D = 4096
HEADS = 16
MESH = pl.DeviceIdType.MESH
F32 = jnp.float32
BF16 = jnp.bfloat16


def tile_of(width):
    return 512 if width % 512 == 0 else (256 if width % 256 == 0 else 128)


def lane_fill(column):
    return jnp.broadcast_to(column, (column.shape[0], 128))


def split_high_low(column):
    high = column.astype(BF16)
    low = (column - high.astype(F32)).astype(BF16)
    return jnp.concatenate([lane_fill(high.astype(F32)), lane_fill(low.astype(F32))], axis=1)


def kernel(
    kv, tp, chunks,
    positions, tokens, state, norm_gain, freq, w_query, w_key, w_value, w_gate, w_out, mlp_gain, w_up, w_down,
    out_ref, st_v,
    pos_s, tok_v, gain1_v, gain2_v, freq_v, wq_v, wk_v, wv_v, wg_v, wo_v, wu_v, wd_v,
    send1, recv1, ret, mix, send2, recv2, sums2, rsums2, hid, down, out_v,
    load_sem, s1_sem, r1_sem, sr_sem, rr_sem, sm_sem, rm_sem, s2_sem, r2_sem, ss_sem, rs_sem, sh_sem, rh_sem,
    sd_sem, rd_sem,
):
    me_kv = lax.axis_index("kv")
    me_tp = lax.axis_index("tp")
    rows, width = tok_v.shape
    seqs = rows // kv
    ret_width = wq_v.shape[1]
    head_size = st_v.shape[-1]
    heads = st_v.shape[1]
    ff = wu_v.shape[1]
    cw = ff // chunks

    loads = []

    def load(src, dst):
        copy = pltpu.make_async_copy(src, dst, load_sem.at[len(loads)])
        loads.append(copy)
        copy.start()
        return copy

    l_tok = load(tokens, tok_v)
    l_g1 = load(norm_gain, gain1_v)
    l_w = [load(a, b) for a, b in ((w_query, wq_v), (w_key, wk_v), (w_value, wv_v), (w_gate, wg_v))]
    l_freq = load(freq, freq_v)
    l_pos = load(positions, pos_s)
    l_state = load(state, st_v)
    l_wo = load(w_out, wo_v)
    l_g2 = load(mlp_gain, gain2_v)
    l_up = [load(w_up.at[:, pl.ds(c * cw, cw)], wu_v.at[:, pl.ds(c * cw, cw)]) for c in range(chunks)]
    l_down = [load(w_down.at[pl.ds(c * cw, cw), :], wd_v.at[pl.ds(c * cw, cw), :]) for c in range(chunks)]

    barrier = pltpu.get_barrier_semaphore()
    for s in range(1, kv):
        pl.semaphore_signal(barrier, inc=1, device_id={"kv": (me_kv + s) % kv}, device_id_type=MESH)
    for s in range(1, tp):
        pl.semaphore_signal(barrier, inc=1, device_id={"tp": lax.rem(me_tp + s, tp)}, device_id_type=MESH)

    upper = (2 * me_kv) // kv

    def offset(s):
        return upper * s + (1 - upper) * (kv - s)

    def remote(src, dst, send_sem, recv_sem, axis, target):
        copy = pltpu.make_async_remote_copy(
            src_ref=src, dst_ref=dst, send_sem=send_sem, recv_sem=recv_sem,
            device_id={axis: target}, device_id_type=MESH,
        )
        copy.start()
        return copy

    l_tok.wait()
    l_g1.wait()
    inputs = tok_v[...].astype(F32)
    normed = (inputs * gain1_v[...]).astype(BF16)
    extra = split_high_low(jnp.sum(inputs * inputs, axis=1, keepdims=True))
    for j in range(kv):
        send1[0, j, :, 2 * ret_width:] = extra[j * seqs:(j + 1) * seqs].astype(BF16)

    l_freq.wait()
    l_pos.wait()
    row = lax.broadcasted_iota(jnp.int32, (seqs, head_size), 0)
    lane = lax.broadcasted_iota(jnp.int32, (seqs, head_size), 1)
    pos = jnp.zeros((seqs, head_size), F32)
    for b in range(seqs):
        pos = jnp.where(row == b, pos_s[b].astype(F32), pos)
    angle = pos * freq_v[...]
    cosine = jnp.cos(angle)
    sine = jnp.where(lane < head_size // 2, -1.0, 1.0) * jnp.sin(angle)

    t1 = tile_of(ret_width)
    copies = ([], [])
    for i, weight in enumerate((wq_v, wk_v, wv_v, wg_v)):
        l_w[i].wait()
        for n in range(ret_width // t1):
            term = jnp.dot(normed, weight[:, n * t1:(n + 1) * t1], preferred_element_type=F32)
            at = (i % 2) * ret_width + n * t1
            for j in range(kv):
                send1[i // 2, j, :, at:at + t1] = term[j * seqs:(j + 1) * seqs].astype(BF16)
        if i % 2 == 1:
            if i == 1:
                pl.semaphore_wait(barrier, kv + tp - 2)
            p = i // 2
            piece = pl.ds(0, 2 * ret_width + (256 if p == 0 else 0))
            for s in range(1, kv):
                to = lax.rem(me_kv + offset(s), kv)
                copies[p].append(
                    remote(
                        send1.at[p, to, :, piece], recv1.at[p, offset(s) - 1, :, piece],
                        s1_sem.at[p, s - 1], r1_sem.at[p, offset(s) - 1], "kv", to,
                    )
                )
    pending = copies[0] + copies[1]

    def gathered(p, size):
        result = send1[p, me_kv, :, :size].astype(F32)
        for s in range(1, kv):
            copies[p][s - 1].wait_recv()
            result = result + recv1[p, offset(s) - 1, :, :size].astype(F32)
        return result

    summed = gathered(0, 2 * ret_width + 256)
    total = summed[:, 2 * ret_width:2 * ret_width + 1] + summed[:, 2 * ret_width + 128:2 * ret_width + 129]
    scale1 = lax.rsqrt(total / D + 1e-06)

    def stack(values, i):
        base = i * ret_width
        return jnp.concatenate(
            [values[:, base + h * head_size:base + (h + 1) * head_size] * scale1 for h in range(heads)], axis=0
        )

    cos_all = jnp.concatenate([cosine] * heads, axis=0)
    sin_all = jnp.concatenate([sine] * heads, axis=0)

    def turn(x):
        return x * cos_all + pltpu.roll(x, head_size // 2, 1) * sin_all

    count = seqs * heads
    query = turn(stack(summed, 0))
    key = turn(stack(summed, 1)) * head_size ** (-0.5)
    columns = jnp.transpose(
        jnp.concatenate([query, key, jnp.zeros((128 - 2 * count, head_size), F32)], axis=0)
    )
    overlap = jnp.sum(query * key, axis=1, keepdims=True)
    gammas = [
        1.0 - jnp.exp2(jnp.full((1, head_size), -5.0, F32) - 5.0 * (me_tp * heads + h).astype(F32) / (HEADS - 1))
        for h in range(heads)
    ]
    l_state.wait()
    old_reads = []
    for h in range(heads):
        for b in range(seqs):
            at = h * seqs + b
            old_reads.append(gammas[h] * jnp.sum(columns[:, at:at + 1] * st_v[b, h], axis=0, keepdims=True))
    old_read = jnp.concatenate(old_reads, axis=0)
    summed = gathered(1, 2 * ret_width)
    value = stack(summed, 0)
    gate = stack(summed, 1)
    read = old_read + overlap * value
    read = read * lax.rsqrt(jnp.mean(read * read, axis=-1, keepdims=True) + 1e-06)
    kept = read * (gate / (1.0 + jnp.exp(-gate)))
    for h in range(heads):
        ret[me_kv, :, h * head_size:(h + 1) * head_size] = kept[h * seqs:(h + 1) * seqs].astype(BF16)
    copies = []
    for s in range(1, kv):
        to = lax.rem(me_kv + offset(s), kv)
        copies.append(remote(ret.at[me_kv], ret.at[me_kv], sr_sem.at[s - 1], rr_sem.at[offset(s) - 1], "kv", to))
    pending += copies
    for h in range(heads):
        for b in range(seqs):
            at = h * seqs + b
            st_v[b, h] = gammas[h] * st_v[b, h] + columns[:, count + at:count + at + 1] * value[at:at + 1, :]

    t2 = tile_of(width)
    l_wo.wait()
    mix_copies = []
    for r in range(kv):
        owner = me_kv if r == 0 else lax.rem(me_kv + kv - offset(r), kv)
        if r > 0:
            copies[r - 1].wait_recv()
        block = ret[owner]
        for n in range(width // t2):
            cols = slice(n * t2, (n + 1) * t2)
            mix[me_tp, owner, :, cols] = jnp.dot(block, wo_v[:, cols], preferred_element_type=F32).astype(BF16)
        row_copies = []
        for s in range(1, tp):
            to = lax.rem(me_tp + s, tp)
            row_copies.append(
                remote(
                    mix.at[me_tp, owner], mix.at[me_tp, owner], sm_sem.at[r, s - 1], rm_sem.at[r, s - 1], "tp", to
                )
            )
        mix_copies.append(row_copies)
        pending += row_copies
    for row_copies in mix_copies:
        for copy in row_copies:
            copy.wait_recv()

    def added(j):
        return jnp.concatenate([mix[j, k].astype(F32) for k in range(kv)], axis=0)

    head_sum = added(0)
    for j in range(1, tp):
        head_sum = head_sum + added(j)
    mixed = (inputs + head_sum).astype(BF16)
    middle = mixed.astype(F32)
    l_g2.wait()
    normed2 = (middle * gain2_v[...]).astype(BF16)
    extra = split_high_low(jnp.sum(middle * middle, axis=1, keepdims=True))
    for j in range(kv):
        sums2[j] = extra[j * seqs:(j + 1) * seqs].astype(BF16)
    sum_copies = []
    for s in range(1, kv):
        to = lax.rem(me_kv + offset(s), kv)
        sum_copies.append(remote(sums2.at[to], rsums2.at[offset(s) - 1], ss_sem.at[s - 1], rs_sem.at[offset(s) - 1], "kv", to))
    pending += sum_copies

    t3 = tile_of(cw)
    up_copies = []
    for c in range(chunks):
        l_up[c].wait()

        @pl.loop(0, cw // t3)
        def _(n, c=c):
            start = pl.multiple_of(n * t3, t3)
            term = jnp.dot(normed2, wu_v[:, pl.ds(c * cw + start, t3)], preferred_element_type=F32)
            for j in range(kv):
                send2[c, j, :, pl.ds(start, t3)] = term[j * seqs:(j + 1) * seqs].astype(BF16)

        row_copies = []
        for s in range(1, kv):
            to = lax.rem(me_kv + offset(s), kv)
            row_copies.append(
                remote(send2.at[c, to], recv2.at[c, offset(s) - 1], s2_sem.at[c, s - 1], r2_sem.at[c, offset(s) - 1], "kv", to)
            )
        up_copies.append(row_copies)
        pending += row_copies

    sums = sums2[me_kv].astype(F32)
    for s in range(1, kv):
        sum_copies[s - 1].wait_recv()
        sums = sums + rsums2[offset(s) - 1].astype(F32)
    scale2 = lax.rsqrt((sums[:, :1] + sums[:, 128:129]) / D + 1e-06)

    hid_copies = []
    for c in range(chunks):
        up_sum = send2[c, me_kv].astype(F32)
        for s in range(1, kv):
            up_copies[c][s - 1].wait_recv()
            up_sum = up_sum + recv2[c, offset(s) - 1].astype(F32)
        positive = jnp.maximum(up_sum * scale2, 0.0)
        hid[c, me_kv] = (positive * positive).astype(BF16)
        row_copies = []
        for s in range(1, kv):
            to = lax.rem(me_kv + offset(s), kv)
            row_copies.append(
                remote(hid.at[c, me_kv], hid.at[c, me_kv], sh_sem.at[c, s - 1], rh_sem.at[c, offset(s) - 1], "kv", to)
            )
        hid_copies.append(row_copies)
        pending += row_copies

    last = []
    for c in range(chunks):
        l_down[c].wait()
        for s in range(1, kv):
            hid_copies[c][s - 1].wait_recv()
        hidden = jnp.concatenate([hid[c, j].astype(F32) for j in range(kv)], axis=0).astype(BF16)
        for n in range(width // t2):
            cols = slice(n * t2, (n + 1) * t2)
            term = jnp.dot(hidden, wd_v[c * cw:(c + 1) * cw, cols], preferred_element_type=F32)
            if c > 0:
                term = term + out_v[:, cols]
            if c < chunks - 1:
                out_v[:, cols] = term
                continue
            down[me_tp, n] = term.astype(BF16)
            row_copies = []
            for s in range(1, tp):
                to = lax.rem(me_tp + s, tp)
                row_copies.append(
                    remote(
                        down.at[me_tp, n], down.at[me_tp, n], sd_sem.at[n, s - 1], rd_sem.at[n, s - 1], "tp", to
                    )
                )
            last.append(row_copies)
            pending += row_copies
    for n in range(width // t2):
        for copy in last[n]:
            copy.wait_recv()
        total = down[0, n].astype(F32)
        for j in range(1, tp):
            total = total + down[j, n].astype(F32)
        cols = slice(n * t2, (n + 1) * t2)
        out_ref[:, cols] = (middle[:, cols] + total).astype(BF16)
    for copy in pending:
        copy.wait_send()


def finish(made, fresh, out_ref, new_state, sem):
    first = pltpu.make_async_copy(fresh, new_state, sem.at[0])
    second = pltpu.make_async_copy(made, out_ref, sem.at[1])
    first.start()
    second.start()
    first.wait()
    second.wait()


def solution(mesh):
    kv, tp = mesh.shape["kv"], mesh.shape["tp"]

    def shards(
        tokens, positions, state, norm_gain, w_query, w_key, w_value, w_gate, w_out, mlp_gain, w_up, w_down
    ):
        rows, width = tokens.shape
        seqs, heads, head_size, _ = state.shape
        ret_width = w_query.shape[1]
        ff = w_up.shape[1]
        chunks = 4
        cw = ff // chunks
        half = head_size // 2
        table = 10000.0 ** (-(np.arange(half) * 2.0) / head_size)
        freq = jnp.asarray(np.concatenate([table, table])[None, :], F32)
        any_spec = pl.BlockSpec(memory_space=pltpu.HBM)
        vmem = pltpu.VMEM
        dma = pltpu.SemaphoreType.DMA
        block1 = 2 * ret_width + 256
        parts = width // tile_of(width)
        made, fresh = pl.pallas_call(
            functools.partial(kernel, kv, tp, chunks),
            name="layer",
            out_shape=(
                pltpu.VMEM((rows, width), BF16),
                pltpu.VMEM(state.shape, F32),
            ),
            in_specs=[any_spec] * 13,
            out_specs=(pl.BlockSpec(memory_space=pltpu.VMEM), pl.BlockSpec(memory_space=pltpu.VMEM)),
            scratch_shapes=[
                pltpu.SMEM(positions.shape, jnp.int32),
                vmem((rows, width), BF16),
                vmem((1, width), F32),
                vmem((1, width), F32),
                vmem((1, head_size), F32),
                vmem(w_query.shape, BF16),
                vmem(w_key.shape, BF16),
                vmem(w_value.shape, BF16),
                vmem(w_gate.shape, BF16),
                vmem(w_out.shape, BF16),
                vmem(w_up.shape, BF16),
                vmem(w_down.shape, BF16),
                vmem((2, kv, seqs, block1), BF16),
                vmem((2, kv - 1, seqs, block1), BF16),
                vmem((kv, seqs, ret_width), BF16),
                vmem((tp, kv, seqs, width), BF16),
                vmem((chunks, kv, seqs, cw), BF16),
                vmem((chunks, kv - 1, seqs, cw), BF16),
                vmem((kv, seqs, 256), BF16),
                vmem((kv - 1, seqs, 256), BF16),
                vmem((chunks, kv, seqs, cw), BF16),
                vmem((tp, parts, rows, width // parts), BF16),
                vmem((rows, width), F32),
                dma((11 + 2 * chunks,)),
                dma((2, kv - 1)), dma((2, kv - 1)),
                dma((kv - 1,)), dma((kv - 1,)),
                dma((kv, tp - 1)), dma((kv, tp - 1)),
                dma((chunks, kv - 1)), dma((chunks, kv - 1)),
                dma((kv - 1,)), dma((kv - 1,)),
                dma((chunks, kv - 1)), dma((chunks, kv - 1)),
                dma((parts, tp - 1)), dma((parts, tp - 1)),
            ],
            compiler_params=pltpu.CompilerParams(
                collective_id=0, has_side_effects=True, vmem_limit_bytes=48 * 1024 * 1024
            ),
        )(
            *[
                pltpu.with_memory_space_constraint(x, pltpu.HBM)
                for x in (
                    positions, tokens, state, norm_gain[None, :], freq, w_query, w_key, w_value, w_gate, w_out,
                    mlp_gain[None, :], w_up, w_down,
                )
            ],
        )
        return pl.pallas_call(
            finish,
            name="finish",
            out_shape=(
                jax.ShapeDtypeStruct((rows, width), BF16),
                jax.ShapeDtypeStruct(state.shape, F32),
            ),
            in_specs=[pl.BlockSpec(memory_space=pltpu.VMEM)] * 2,
            out_specs=(any_spec, any_spec),
            scratch_shapes=[pltpu.SemaphoreType.DMA((2,))],
            compiler_params=pltpu.CompilerParams(vmem_limit_bytes=4 * 1024 * 1024),
        )(made, fresh)

    return jax.shard_map(
        shards,
        mesh=mesh,
        in_specs=(
            P("grp", "kv"),
            P(("grp", "kv")),
            P(("grp", "kv"), "tp", None, None),
            P("kv"),
            P("kv", "tp"),
            P("kv", "tp"),
            P("kv", "tp"),
            P("kv", "tp"),
            P("tp", "kv"),
            P("kv"),
            P("kv", "tp"),
            P("tp", "kv"),
        ),
        out_specs=(P("grp", "kv"), P(("grp", "kv"), "tp", None, None)),
        check_vma=False,
    )
```
